32 devices in a mesh: ep: 8 (over z, x), tp: 4 (over y, core).
Axes of the slice: x: 2, y: 2, z: 4, core: 2. Of those that a mesh axis runs over, the one named last changes fastest.
Arguments:
- query_rows: bfloat16 [3072, 4096], P('ep', 'tp'), may hold values from -6 to 6
- key_rows: bfloat16 [3072, 2048], P('ep', 'tp'), may hold values from -6 to 6
- value_rows: bfloat16 [3072, 2048], P('ep', 'tp'), may hold values from -6 to 6
- query_gain: float32 [128], replicated, may hold values from 0.4 to 5
- key_gain: float32 [128], replicated, may hold values from 0.4 to 5
- w_out: bfloat16 [4096, 2048], P('tp'), may hold values from -0.09375 to 0.09375
- mixer_gain: float32 [2048], replicated, may hold values from 0.1 to 1.9
- expert_input: bfloat16 [1536, 2048], P('ep'), may hold values from -6 to 6
- expert_ids: int32 [1536, 2], P('ep'), may hold values from 0 to 7, as said below
- expert_weights: float32 [1536, 2], P('ep'), may hold values from 0.1 to 1
- input_gain: float32 [2048], replicated, may hold values from 0.1 to 1.9
- w_gate: bfloat16 [8, 2048, 4096], P('ep', None, 'tp'), may hold values from -0.125 to 0.125
- w_up: bfloat16 [8, 2048, 4096], P('ep', None, 'tp'), may hold values from -0.125 to 0.125
- w_down: bfloat16 [8, 4096, 2048], P('ep', 'tp'), may hold values from -2 to 2
- out_gain: float32 [2048], P('tp'), may hold values from 0.1 to 1.9
Outputs:
- mixer_result: bfloat16 [3072, 2048], P(('ep', 'tp'))
- moe_result: bfloat16 [1536, 2048], P('ep', 'tp')
The draws below stay inside these ranges and needn't reach their ends.
Inputs may be any that keep to these rules, and one draw needn't show every extreme that they name: `expert_ids`: the two experts of a row differ and lie in one group of 2 consecutive experts. Among the rows of one index of ep (aligned blocks of 192 rows) no expert is named by more than 72 rows, and in every block some expert is named by exactly 72 rows.
All inputs are finite; a program needn't handle non-finite values.
Results may differ from the reference program's by a relative error of at most 0.02.
The reference program's roundings to bfloat16 on the way count: a program that leaves them out, or rounds other values in their place, can miss the bound.
Values may be sent and summed in bfloat16 or wider, within the bound.
No kernel may reach another device: no remote copies, remote signals or barrier semaphores. Data moves between devices by JAX's collectives and lax.ppermute only.
A program may use at most 64 MiB of HBM per device.

```python
import math
import jax
import jax.numpy as jnp
from jax import lax

D = 2048
HEADS = 32
KV_HEADS = 16
HEAD = 128
GRID = 64
FF = 4096
GROUPS = 4
TOP = 2
ROWS2 = 192
EXPERTS = 8
INNER = 2
CAP = 72
TOK1 = 3072
TOK2 = 1536
N_EP = 8
N_TP = 4


def key_field(key):
    normal_base = jax.random.normal(jax.random.fold_in(key, 11), (TOK1, KV_HEADS * HEAD), jnp.float32)
    return jnp.clip(normal_base, -6.0, 6.0)


def draw_key_rows(key, part):
    return key_field(key).astype(jnp.bfloat16)


def draw_query_rows(key, part):
    fresh = jax.random.normal(jax.random.fold_in(key, 12), (TOK1, HEADS * HEAD), jnp.float32)
    return jnp.clip(fresh, -6.0, 6.0).astype(jnp.bfloat16)


def gain_field(key, offset):
    return jax.random.uniform(jax.random.fold_in(key, offset), (HEAD,), jnp.float32, 0.4, 1.6)


def draw_query_gain(key, part):
    return gain_field(key, 31)


def draw_key_gain(key, part):
    return gain_field(key, 32)


def draw_w_down(key, part):
    normal_base = jax.random.normal(jax.random.fold_in(key, 21), (EXPERTS, FF, D), jnp.float32) * FF ** (-0.5)
    column_ramp = jnp.exp(2.3 * jnp.arange(D, dtype=jnp.float32) / D)
    jitter = jax.random.uniform(jax.random.fold_in(key, 22), (D,), jnp.float32, 0.5, 1.5)
    return jnp.clip(normal_base * column_ramp * jitter, -2.0, 2.0).astype(jnp.bfloat16)


def block_ids(block_key):
    eighth = ROWS2 // 8
    shares = jnp.array([1, 2, 2, 3], jnp.int32)[jax.random.permutation(jax.random.fold_in(block_key, 1), 4)]
    group_sizes = shares * eighth
    group_ends = jnp.cumsum(group_sizes)
    starts = group_ends - group_sizes
    row_order = jnp.arange(ROWS2, dtype=jnp.int32)
    group_of = jnp.sum((row_order[:, None] >= group_ends[None, :]).astype(jnp.int32), axis=1)
    within = row_order - starts[group_of]
    shifts = jax.random.randint(jax.random.fold_in(block_key, 2), (GROUPS,), 1, INNER)
    labels = jax.vmap(lambda offset: jax.random.permutation(jax.random.fold_in(block_key, offset), INNER))(jnp.arange(GROUPS) + 3)
    first_pick = labels[group_of, within % INNER]
    second_pick = labels[group_of, (within + shifts[group_of]) % INNER]
    chosen_ids = jnp.stack([first_pick, second_pick], axis=1) + INNER * group_of[:, None]
    shuffle = jax.random.permutation(jax.random.fold_in(block_key, 9), ROWS2)
    return chosen_ids[shuffle].astype(jnp.int32)


def draw_expert_ids(key, part):
    block_keys = jax.vmap(lambda block_index: jax.random.fold_in(key, block_index))(jnp.arange(N_EP) + 100)
    return jax.vmap(block_ids)(block_keys).reshape(TOK2, TOP)


def shard_levels(own_key, dims, shards, smallest, top_value):
    loudness, own = 1.0, jax.random.fold_in(own_key, 6)
    for dim, parts in shards:
        steps = jnp.exp(jax.random.uniform(jax.random.fold_in(own, dim), (parts,), jnp.float32, smallest / len(shards), top_value / len(shards)))
        loudness = loudness * jnp.repeat(steps, dims[dim] // parts).reshape([-1 if axis == dim else 1 for axis in range(len(dims))])
    return loudness


def scatter_about(rng, dims, width, reach, pieces=(), held_as=jnp.bfloat16):
    level = shard_levels(rng, dims, pieces, -0.22, 0.18) if pieces else 1.0
    drawn = jax.random.normal(rng, dims, jnp.float32) * width * level
    return jnp.minimum(jnp.maximum(drawn, -reach), reach).astype(held_as)


def setup_inputs(seed: int = 0) -> dict:
    key_list = jax.random.split(jax.random.key(seed), 16)
    query_rows = draw_query_rows(jax.random.fold_in(key_list[15], 71), 0)
    key_rows = draw_key_rows(jax.random.fold_in(key_list[15], 71), 0)
    value_rows = scatter_about(key_list[2], (TOK1, KV_HEADS * HEAD), 1.0, 6.0, ((0, 8), (1, 4)))
    query_gain = draw_query_gain(jax.random.fold_in(key_list[15], 71), 0)
    key_gain = draw_key_gain(jax.random.fold_in(key_list[15], 71), 0)
    w_out = scatter_about(key_list[5], (HEADS * HEAD, D), (HEADS * HEAD) ** -0.5, 0.09375, ((0, 4),))
    mixer_gain = jnp.clip(1.0 + 0.18 * jax.random.normal(key_list[6], (D,), jnp.float32), 0.1, 1.9)
    expert_input = scatter_about(key_list[7], (TOK2, D), 1.0, 6.0, ((0, 8),))
    expert_ids = draw_expert_ids(jax.random.fold_in(key_list[15], 71), 0)
    expert_weights = jnp.clip(jnp.exp(math.log(1.0) - 2.3025851 * jax.random.uniform(key_list[9], (TOK2, TOP), jnp.float32) ** shard_levels(key_list[9], (TOK2, TOP), ((0, 8),), -0.2, 0.2)), 0.1, 1.0)
    input_gain = jnp.clip(1.0 + 0.18 * jax.random.normal(key_list[10], (D,), jnp.float32), 0.1, 1.9)
    w_gate = scatter_about(key_list[11], (EXPERTS, D, FF), D ** -0.5, 0.125, ((0, 8), (2, 4)))
    w_up = scatter_about(key_list[12], (EXPERTS, D, FF), D ** -0.5, 0.125, ((0, 8), (2, 4)))
    w_down = draw_w_down(jax.random.fold_in(key_list[15], 71), 0)
    out_gain = jnp.clip(1.0 + 0.18 * jax.random.normal(key_list[14], (D,), jnp.float32), 0.1, 1.9)
    return {"query_rows": query_rows, "key_rows": key_rows, "value_rows": value_rows, "query_gain": query_gain, "key_gain": key_gain, "w_out": w_out, "mixer_gain": mixer_gain, "expert_input": expert_input, "expert_ids": expert_ids, "expert_weights": expert_weights, "input_gain": input_gain, "w_gate": w_gate, "w_up": w_up, "w_down": w_down, "out_gain": out_gain}


EPS = 1e-06
THETA = 10000.0

def turn_half(half_part, position):
    half_width = half_part.shape[-1]
    frequency = THETA ** (-jnp.arange(0, half_width, 2, dtype=jnp.float32) / half_width)
    angles = position[:, None, None] * frequency[None, None, :]
    cosine = jnp.cos(angles)
    sine_part = jnp.sin(angles)
    first_half = half_part[..., :half_width // 2]
    second = half_part[..., half_width // 2:]
    return jnp.concatenate([first_half * cosine - second * sine_part, second * cosine + first_half * sine_part], axis=-1)

def norm_turn(raw_rows, gain_vec, row_offset):
    row_count = raw_rows.shape[0]
    head_dim = gain_vec.shape[0]
    head_count = raw_rows.shape[1] // head_dim
    by_head = raw_rows.astype(jnp.float32).reshape(row_count, head_count, head_dim)
    scaled = by_head * lax.rsqrt(lax.optimization_barrier(jnp.mean(by_head * by_head, axis=-1, keepdims=True)) + EPS) * gain_vec
    position = row_offset + jnp.arange(row_count, dtype=jnp.int32)
    grid_row = (position // GRID).astype(jnp.float32)
    grid_col = (position % GRID).astype(jnp.float32)
    half_dim = head_dim // 2
    turned = jnp.concatenate([turn_half(scaled[..., :half_dim], grid_row), turn_half(scaled[..., half_dim:], grid_col)], axis=-1)
    return turned.reshape(row_count, head_count * head_dim).astype(jnp.bfloat16)

def mixer_ref(query_rows, key_rows, value_rows, query_gain, key_gain, w_out, mixer_gain):
    token_count = query_rows.shape[0]
    group_size = HEADS // KV_HEADS
    query_turned = norm_turn(query_rows, query_gain, 0)
    key_turned = norm_turn(key_rows, key_gain, 0)
    query_heads = query_turned.reshape(token_count, HEADS, HEAD).transpose(1, 0, 2)
    key_heads = jnp.repeat(key_turned.reshape(token_count, KV_HEADS, HEAD).transpose(1, 0, 2), group_size, axis=0)
    value_heads = jnp.repeat(value_rows.reshape(token_count, KV_HEADS, HEAD).transpose(1, 0, 2), group_size, axis=0)

    def one_head(head_triple):
        query_head, key_head, value_head = head_triple
        scores = jnp.dot(query_head, key_head.T, preferred_element_type=jnp.float32) * HEAD ** (-0.5)
        row_max = lax.optimization_barrier(jnp.max(scores, axis=1, keepdims=True))
        exponent = jnp.exp(scores - row_max)
        probs = exponent.astype(jnp.bfloat16)
        numer = jnp.dot(probs, value_head, preferred_element_type=jnp.float32)
        return (numer / lax.optimization_barrier(jnp.sum(exponent, axis=1, keepdims=True))).astype(jnp.bfloat16)
    attended = lax.map(one_head, (query_heads, key_heads, value_heads))
    attended = attended.transpose(1, 0, 2).reshape(token_count, HEADS * HEAD)
    block_width = HEADS * HEAD // N_TP
    attended_blocks = attended.reshape(token_count, N_TP, block_width).transpose(1, 0, 2)
    weight_blocks = w_out.reshape(N_TP, block_width, D)

    def add_part(running_sum, block_pair):
        attended_block, weight_block = block_pair
        head_part = jnp.dot(attended_block, weight_block, preferred_element_type=jnp.float32).astype(jnp.bfloat16)
        head_part = lax.optimization_barrier(head_part)
        return (running_sum + head_part.astype(jnp.float32), None)
    mixed_sum, _ = lax.scan(add_part, jnp.zeros((token_count, D), jnp.float32), (attended_blocks, weight_blocks))
    scaled = mixed_sum * lax.rsqrt(lax.optimization_barrier(jnp.mean(mixed_sum * mixed_sum, axis=1, keepdims=True)) + EPS) * mixer_gain
    return scaled.astype(jnp.bfloat16)

def expert_ref(expert_input, expert_ids, expert_weights, input_gain, w_gate, w_up, w_down, out_gain):
    token_count = expert_input.shape[0]
    inputs_f = expert_input.astype(jnp.float32)
    normed = (inputs_f * lax.rsqrt(lax.optimization_barrier(jnp.mean(inputs_f * inputs_f, axis=1, keepdims=True)) + EPS) * input_gain).astype(jnp.bfloat16)
    padded = jnp.concatenate([normed, jnp.zeros((1, D), jnp.bfloat16)], axis=0)
    flat_ids = expert_ids.reshape(-1)
    pick_count = flat_ids.shape[0]
    top_count = expert_ids.shape[1]
    weight_flat = jnp.concatenate([expert_weights.reshape(-1), jnp.zeros((1,), jnp.float32)])
    slot_total = N_EP * CAP
    block_width = FF // N_TP

    def one_expert(accum, expert_index):
        chosen = flat_ids == expert_index
        position = jnp.cumsum(chosen.astype(jnp.int32)) - 1
        target = jnp.where(chosen, position, slot_total).astype(jnp.int32)
        pick_table = jnp.full((slot_total,), pick_count, jnp.int32).at[target].set(jnp.arange(pick_count, dtype=jnp.int32), mode='drop')
        token_table = (pick_table // top_count).astype(jnp.int32)
        gathered = jnp.take(padded, token_table, axis=0)
        gate_weight = lax.dynamic_index_in_dim(w_gate, expert_index, 0, keepdims=False)
        up_weight = lax.dynamic_index_in_dim(w_up, expert_index, 0, keepdims=False)
        down_weight = lax.dynamic_index_in_dim(w_down, expert_index, 0, keepdims=False)
        gate_pre = jnp.dot(gathered, gate_weight, preferred_element_type=jnp.float32)
        up_pre = jnp.dot(gathered, up_weight, preferred_element_type=jnp.float32)
        hidden = (jax.nn.silu(gate_pre) * up_pre).astype(jnp.bfloat16)
        hidden_blocks = hidden.reshape(slot_total, N_TP, block_width).transpose(1, 0, 2).astype(jnp.float32)
        down_blocks = down_weight.reshape(N_TP, block_width, D).astype(jnp.float32)
        expert_part = jnp.einsum('jsf,jfd->jsd', hidden_blocks, down_blocks).astype(jnp.bfloat16)
        expert_part = lax.optimization_barrier(expert_part)
        expert_rows = lax.optimization_barrier(jnp.sum(expert_part.astype(jnp.float32), axis=0)).astype(jnp.bfloat16)
        weights_now = jnp.take(weight_flat, pick_table)
        accum = accum.at[token_table].add(weights_now[:, None] * expert_rows.astype(jnp.float32), mode='drop')
        return (accum, None)
    combined, _ = lax.scan(one_expert, jnp.zeros((token_count, D), jnp.float32), jnp.arange(EXPERTS, dtype=jnp.int32))
    scaled = combined * lax.rsqrt(lax.optimization_barrier(jnp.mean(combined * combined, axis=1, keepdims=True)) + EPS) * out_gain
    return scaled.astype(jnp.bfloat16)

def reference(query_rows, key_rows, value_rows, query_gain, key_gain, w_out, mixer_gain, expert_input, expert_ids, expert_weights, input_gain, w_gate, w_up, w_down, out_gain):
    mixer_result = mixer_ref(query_rows, key_rows, value_rows, query_gain, key_gain, w_out, mixer_gain)
    moe_result = expert_ref(expert_input, expert_ids, expert_weights, input_gain, w_gate, w_up, w_down, out_gain)
    return (mixer_result, moe_result)
```

```python
import functools
import math

import jax
import jax.numpy as jnp
import numpy as np
from jax import lax
from jax.experimental import pallas as pl
from jax.experimental.pallas import tpu as pltpu
from jax.sharding import PartitionSpec as P

GRID = 64
GROUPS = 4


EPS = 1e-06
THETA = 10000.0


def turn_half(half_part, position):
    half_width = half_part.shape[-1]
    frequency = THETA ** (-jnp.arange(0, half_width, 2, dtype=jnp.float32) / half_width)
    angles = position[:, None, None] * frequency[None, None, :]
    cosine = jnp.cos(angles)
    sine_part = jnp.sin(angles)
    first_half = half_part[..., : half_width // 2]
    second = half_part[..., half_width // 2 :]
    return jnp.concatenate(
        [first_half * cosine - second * sine_part, second * cosine + first_half * sine_part],
        axis=-1,
    )


def norm_turn(raw_rows, gain_vec, row_offset):
    row_count = raw_rows.shape[0]
    head_dim = gain_vec.shape[0]
    head_count = raw_rows.shape[1] // head_dim
    by_head = raw_rows.astype(jnp.float32).reshape(row_count, head_count, head_dim)
    scaled = (
        by_head * lax.rsqrt(jnp.mean(by_head * by_head, axis=-1, keepdims=True) + EPS) * gain_vec
    )
    position = row_offset + jnp.arange(row_count, dtype=jnp.int32)
    grid_row = (position // GRID).astype(jnp.float32)
    grid_col = (position % GRID).astype(jnp.float32)
    half_dim = head_dim // 2
    turned = jnp.concatenate(
        [turn_half(scaled[..., :half_dim], grid_row), turn_half(scaled[..., half_dim:], grid_col)],
        axis=-1,
    )
    return turned.reshape(row_count, head_count * head_dim).astype(jnp.bfloat16)


def mixer_half(query_rows, key_rows, value_rows, query_gain, key_gain, w_out, mixer_gain):
    row_count = query_rows.shape[0]
    head_dim = query_gain.shape[0]
    row_offset = lax.axis_index("ep") * row_count
    query_turned = norm_turn(query_rows, query_gain, row_offset)
    key_turned = norm_turn(key_rows, key_gain, row_offset)
    local_kv = key_rows.shape[1] // head_dim
    group_size = query_rows.shape[1] // key_rows.shape[1]
    lane_count = group_size * row_count
    grouped = (
        query_turned.reshape(row_count, local_kv, group_size, head_dim)
        .transpose(1, 2, 0, 3)
        .reshape(local_kv, lane_count, head_dim)
    )
    scaling = head_dim ** (-0.5)

    def attend_block(carry, block_pair):
        running_max, running_sum, weighted = carry
        key_block, value_block = block_pair
        scores = (
            jnp.einsum("gqd,ngd->gqn", grouped, key_block, preferred_element_type=jnp.float32)
            * scaling
        )
        new_max = jnp.maximum(running_max, jnp.max(scores, axis=-1))
        exponent = jnp.exp(scores - new_max[..., None])
        factor = jnp.exp(running_max - new_max)
        running_sum = running_sum * factor + jnp.sum(exponent, axis=-1)
        weighted = weighted * factor[..., None] + jnp.einsum(
            "gqn,ngd->gqd",
            exponent.astype(jnp.bfloat16),
            value_block,
            preferred_element_type=jnp.float32,
        )
        return ((new_max, running_sum, weighted), None)

    initial = (
        jnp.full((local_kv, lane_count), -1e30, jnp.float32),
        jnp.zeros((local_kv, lane_count), jnp.float32),
        jnp.zeros((local_kv, lane_count, head_dim), jnp.float32),
    )
    carry = initial
    key_piece = lax.all_gather(key_turned, "ep", axis=0, tiled=True)
    value_piece = lax.all_gather(value_rows, "ep", axis=0, tiled=True)
    piece_rows = key_piece.shape[0]
    block_rows = 512
    block_count = piece_rows // block_rows
    key_split = key_piece.reshape(block_count, block_rows, local_kv, head_dim)
    value_split = value_piece.reshape(block_count, block_rows, local_kv, head_dim)
    carry, _ = lax.scan(attend_block, carry, (key_split, value_split))
    running_max, running_sum, weighted = carry
    attended = (weighted / running_sum[..., None]).astype(jnp.bfloat16)
    attended = (
        attended.reshape(local_kv, group_size, row_count, head_dim)
        .transpose(2, 0, 1, 3)
        .reshape(row_count, local_kv * group_size * head_dim)
    )
    mixed_sum = lax.psum_scatter(
        jnp.dot(attended, w_out, preferred_element_type=jnp.float32).astype(jnp.bfloat16),
        "tp",
        scatter_dimension=0,
        tiled=True,
    ).astype(jnp.float32)
    scaled = (
        mixed_sum
        * lax.rsqrt(jnp.mean(mixed_sum * mixed_sum, axis=1, keepdims=True) + EPS)
        * mixer_gain
    )
    return scaled.astype(jnp.bfloat16)


def expert_half(
    expert_input, expert_ids, expert_weights, input_gain, w_gate, w_up, w_down, out_gain
):
    row_count = expert_input.shape[0]
    top_count = expert_ids.shape[1]
    expert_total = w_gate.shape[0] * lax.axis_size("ep")
    inner_count = expert_total // GROUPS
    capacity = 3 * row_count // (4 * inner_count)
    inputs_f = expert_input.astype(jnp.float32)
    normed = (
        inputs_f
        * lax.rsqrt(jnp.mean(inputs_f * inputs_f, axis=1, keepdims=True) + EPS)
        * input_gain
    ).astype(jnp.bfloat16)
    flat_ids = expert_ids.reshape(-1)
    one_hot = (flat_ids[:, None] == jnp.arange(expert_total, dtype=jnp.int32)[None, :]).astype(
        jnp.int32
    )
    earlier = jnp.cumsum(one_hot, axis=0) - one_hot
    rank_in = jnp.sum(earlier * one_hot, axis=1)
    slot_of = flat_ids * capacity + rank_in
    pick_rows = jnp.arange(flat_ids.shape[0], dtype=jnp.int32) // top_count
    source_row = (
        jnp.full((expert_total * capacity,), row_count, jnp.int32).at[slot_of].set(pick_rows)
    )
    padded = jnp.concatenate([normed, jnp.zeros((1, normed.shape[1]), jnp.bfloat16)], axis=0)
    gate_local = w_gate[0]
    up_local = w_up[0]
    down_local = w_down[0]
    outgoing = jnp.take(padded, source_row, axis=0)
    arrived = lax.all_to_all(outgoing, "ep", split_axis=0, concat_axis=0, tiled=True)
    gate_pre = jnp.dot(arrived, gate_local, preferred_element_type=jnp.float32)
    up_pre = jnp.dot(arrived, up_local, preferred_element_type=jnp.float32)
    hidden = (jax.nn.silu(gate_pre) * up_pre).astype(jnp.bfloat16)
    partial_term = jnp.dot(hidden, down_local, preferred_element_type=jnp.float32)
    summed = lax.psum_scatter(
        partial_term.astype(jnp.bfloat16), "tp", scatter_dimension=1, tiled=True
    )
    returned = lax.all_to_all(summed, "ep", split_axis=0, concat_axis=0, tiled=True)
    picked = (
        jnp.take(returned, slot_of, axis=0)
        .reshape(row_count, top_count, returned.shape[1])
        .astype(jnp.float32)
    )
    combined = jnp.sum(picked * expert_weights[:, :, None], axis=1)
    squares = lax.psum(jnp.sum(combined * combined, axis=1), "tp")
    scaled = combined * lax.rsqrt(squares / expert_input.shape[1] + EPS)[:, None] * out_gain
    return scaled.astype(jnp.bfloat16)


VMEM = pl.BlockSpec(memory_space=pltpu.VMEM)
SMEM = pl.BlockSpec(memory_space=pltpu.SMEM)
F32 = jnp.float32
BF16 = jnp.bfloat16


def contract(lhs, rhs, lhs_dim, rhs_dim):
    return lax.dot_general(
        lhs, rhs, (((lhs_dim,), (rhs_dim,)), ((), ())), preferred_element_type=F32
    )


def call(body, outs, args, flops=0, grid_spec=None, **kwargs):
    return pl.pallas_call(
        body,
        out_shape=[jax.ShapeDtypeStruct(shape, dtype) for shape, dtype in outs],
        in_specs=[SMEM if a.dtype == jnp.int32 and a.ndim == 1 else VMEM for a in args],
        out_specs=[VMEM] * len(outs),
        compiler_params=pltpu.CompilerParams(vmem_limit_bytes=56 * 2**20),
        **kwargs,
    )(*args)


def turn_tables(grid_rows, head_dim):
    half = head_dim // 2
    quarter = half // 2
    frequency = np.float32(THETA) ** (
        -np.arange(0, half, 2, dtype=np.float32) / np.float32(half)
    )
    tables = []
    for count, first in ((grid_rows, True), (GRID, False)):
        angles = np.arange(count, dtype=np.float32)[:, None] * frequency[None, :]
        cosine = np.cos(angles.astype(np.float64)).astype(np.float32)
        sine = np.sin(angles.astype(np.float64)).astype(np.float32)
        zero = np.zeros((count, half), np.float32)
        cos_half = np.concatenate([cosine, cosine], axis=1)
        sin_half = np.concatenate([-sine, sine], axis=1)
        pair = [
            np.concatenate([part, zero] if first else [zero, part], axis=1)
            for part in (cos_half, sin_half)
        ]
        tables += pair
    assert tables[0].shape == (grid_rows, 4 * quarter)
    return [jnp.asarray(table) for table in tables]


def turn_one(raw, gain, cosine, sine):
    head_dim = raw.shape[1]
    z = raw.astype(F32)
    z = z * lax.rsqrt(jnp.mean(z * z, axis=1, keepdims=True) + EPS) * gain
    shift = head_dim // 4
    lane = lax.broadcasted_iota(jnp.int32, z.shape, 1)
    partner = jnp.where(
        lane % (2 * shift) < shift,
        pltpu.roll(z, head_dim - shift, 1),
        pltpu.roll(z, shift, 1),
    )
    return z * cosine + partner * sine


def lane_tables(place, row_cos, row_sin, col_cos, col_sin, rows):
    steps = rows // GRID
    base = place[0] * steps
    cosine, sine = [], []
    for step in range(steps):
        cosine.append(row_cos[pl.ds(base + step, 1), :] + col_cos[...])
        sine.append(row_sin[pl.ds(base + step, 1), :] + col_sin[...])
    return jnp.concatenate(cosine, axis=0), jnp.concatenate(sine, axis=0)


def prep_kv_body(place, k, v, gain, rc, rs, cc, cs, own, other):
    rows = k.shape[0]
    head_dim = gain.shape[1]
    groups = own.shape[1]
    cosine, sine = lane_tables(place, rc, rs, cc, cs, rows)
    for out, half in ((own, place[1]), (other, 1 - place[1])):
        for g in range(groups):
            lanes = pl.ds(pl.multiple_of((half * groups + g) * head_dim, head_dim), head_dim)
            out[0, g] = turn_one(k[:, lanes], gain[...], cosine, sine).astype(BF16)
            out[1, g] = v[:, lanes]


def prep_q_body(place, q, gain, rc, rs, cc, cs, own, other):
    rows = q.shape[0]
    head_dim = gain.shape[1]
    groups, per = own.shape[:2]
    cosine, sine = lane_tables(place, rc, rs, cc, cs, rows)
    for out, half in ((own, place[1]), (other, 1 - place[1])):
        for g in range(groups):
            for h in range(per):
                head = (half * groups + g) * per + h
                lanes = pl.ds(pl.multiple_of(head * head_dim, head_dim), head_dim)
                out[g, h] = turn_one(q[:, lanes], gain[...], cosine, sine).T.astype(BF16)


def attend_body(spec, place, *refs):
    queries, sources, pick, first, last, scale = spec
    q_refs = refs[:queries]
    refs = refs[queries:]
    kv_refs = refs[:sources]
    refs = refs[sources:]
    old = ()
    if not first:
        old, refs = refs[: 3 * queries], refs[3 * queries :]
    groups, per = q_refs[0].shape[:2]
    end = place[2]

    def keys_of(which, g):
        if not pick:
            return [r[which, g] for r in kv_refs]
        near, far = kv_refs[:-1], kv_refs[-1]
        pieces = []
        for i in range(2):
            one = near[i][which, g] if len(near) == 2 else near[0][i, which, g]
            pieces.append(jnp.where(end > 0, far[i, which, g], one))
        return pieces

    def body(g, unused):
        keys = keys_of(0, g)
        values = keys_of(1, g)
        for i, q_ref in enumerate(q_refs):
            for h in range(per):
                q = q_ref[g, h]
                scores = [contract(k, q, 1, 0) for k in keys]
                top = functools.reduce(
                    jnp.maximum, [jnp.max(s, axis=0, keepdims=True) for s in scores]
                )
                if not first:
                    top = jnp.maximum(top, old[3 * i][g, h])
                total, weighted = 0.0, 0.0
                for s, v in zip(scores, values):
                    p = jnp.exp2(s * scale - top * scale)
                    total = total + jnp.sum(p, axis=0, keepdims=True)
                    weighted = weighted + contract(v, p.astype(BF16), 0, 0)
                if not first:
                    factor = jnp.exp2((old[3 * i][g, h] - top) * scale)
                    total = total + old[3 * i + 1][g, h] * factor
                    weighted = weighted + old[3 * i + 2][g, h] * factor
                if last:
                    refs[i][g, h] = (weighted / total).astype(BF16)
                else:
                    refs[3 * i][g, h] = top
                    refs[3 * i + 1][g, h] = total
                    refs[3 * i + 2][g, h] = weighted
        return unused

    lax.fori_loop(0, groups, body, 0)


def attend(place, queries, sources, carry, pick=False, last=False):
    groups, per, head_dim, rows = queries[0].shape
    scale = head_dim**-0.5 * math.log2(math.e)
    stat = ((groups, per, 1, rows), F32)
    if last:
        outs = [((groups, per, head_dim, rows), BF16)] * len(queries)
    else:
        outs = [stat, stat, ((groups, per, head_dim, rows), F32)] * len(queries)
    spec = (len(queries), len(sources), pick, carry is None, last, scale)
    args = [place, *queries, *sources, *([] if carry is None else carry)]
    return call(functools.partial(attend_body, spec), outs, args)


def project_own_body(place, att, w, out):
    rows = att.shape[0]
    half = pl.ds(pl.multiple_of(place[1] * rows, rows), rows)
    out[...] = contract(att[...], w[half, :], 0, 0)


def project_rest_body(place, att, w, base, send, keep, full):
    rows = att.shape[0]
    half = pl.ds(pl.multiple_of((1 - place[1]) * rows, rows), rows)
    full[...] = base[...] + contract(att[...], w[half, :], 0, 0)
    pieces, block = send.shape[:2]
    core = place[4]
    for i in range(pieces):
        theirs = pl.ds(pl.multiple_of((2 * i + 1 - core) * block, block), block)
        mine = pl.ds(pl.multiple_of((2 * i + core) * block, block), block)
        send[i] = full[theirs, :].astype(BF16)
        keep[i] = full[mine, :]


def cross_sum_body(place, mine, theirs, send, keep):
    y = place[3]
    send[...] = (mine[1 - y] + theirs[1 - y].astype(F32)).astype(BF16)
    keep[...] = mine[y] + theirs[y].astype(F32)


def mixer_norm_body(mine, theirs, gain, out):
    mixed = mine[...] + theirs[...].astype(F32)
    mean = jnp.mean(mixed * mixed, axis=1, keepdims=True)
    out[...] = (mixed * lax.rsqrt(mean + EPS) * gain[...]).astype(BF16)


def route_body(inner, capacity, place, x, ids, gain, out, slot_out):
    rows, width = x.shape
    quarter = out.shape[2]
    xf = x[...].astype(F32)
    inverse = lax.rsqrt(jnp.mean(xf * xf, axis=1, keepdims=True) + EPS)
    lanes = pl.ds(pl.multiple_of(place[5] * quarter, quarter), quarter)
    normed = (x[:, lanes].astype(F32) * inverse * gain[:, lanes]).astype(BF16)
    group = ids[:, 0:1] // inner
    in_group = group == lax.broadcasted_iota(jnp.int32, (rows, 128), 1)
    earlier = lax.broadcasted_iota(jnp.int32, (rows, rows), 0) > lax.broadcasted_iota(
        jnp.int32, (rows, rows), 1
    )
    rank = contract(earlier.astype(BF16), in_group.astype(BF16), 1, 0)
    rank = jnp.sum(jnp.where(in_group, rank, 0.0), axis=1, keepdims=True).astype(jnp.int32)
    slot = group * capacity + rank
    slot_out[...] = slot
    slots = GROUPS * capacity
    chosen = (slot == lax.broadcasted_iota(jnp.int32, (rows, slots), 1)).astype(BF16)
    sorted_rows = contract(chosen, normed, 0, 0).astype(BF16)
    for g in range(GROUPS):
        for twin in range(inner):
            out[g * inner + twin] = sorted_rows[g * capacity : (g + 1) * capacity]


def hidden_body(place, own, by_core, by_y, by_both, gate, up, out):
    quarter = own.shape[1]
    y, core = place[3], place[4]
    order = (2 * y + core, 2 * y + 1 - core, 2 * (1 - y) + core, 2 * (1 - y) + 1 - core)
    gate_pre, up_pre = 0.0, 0.0
    for ref, index in zip((own, by_core, by_y, by_both), order):
        part = pl.ds(pl.multiple_of(index * quarter, quarter), quarter)
        rows = ref[...]
        gate_pre = gate_pre + contract(rows, gate[part, :], 1, 0)
        up_pre = up_pre + contract(rows, up[part, :], 1, 0)
    out[...] = (gate_pre / (1.0 + jnp.exp(-gate_pre)) * up_pre).astype(BF16)


def hidden_rows(place, pieces, gate, up, block):
    rows, quarter = pieces[0].shape
    depth, width = gate.shape
    whole = pl.BlockSpec((rows, quarter), lambda i, p: (0, 0))
    strip = pl.BlockSpec((depth, block), lambda i, p: (0, i))
    return pl.pallas_call(
        hidden_body,
        out_shape=jax.ShapeDtypeStruct((rows, width), BF16),
        grid_spec=pltpu.PrefetchScalarGridSpec(
            num_scalar_prefetch=1,
            grid=(width // block,),
            in_specs=[whole] * 4 + [strip] * 2,
            out_specs=pl.BlockSpec((rows, block), lambda i, p: (0, i)),
        ),
        compiler_params=pltpu.CompilerParams(vmem_limit_bytes=56 * 2**20),
    )(place, *pieces, gate, up)


def down_body(place, hidden, down, out):
    out[0] = contract(hidden[...], down[...], 1, 0).astype(out.dtype)


def down_rows(place, hidden, down, theirs, dtype):
    rows, depth = hidden.shape
    block = down.shape[1] // 4
    if theirs:
        column = lambda i, p: (0, 2 * i + 1 - p[4])
    else:
        column = lambda i, p: (0, 2 * i + p[4])
    return pl.pallas_call(
        down_body,
        out_shape=jax.ShapeDtypeStruct((2, rows, block), dtype),
        grid_spec=pltpu.PrefetchScalarGridSpec(
            num_scalar_prefetch=1,
            grid=(2,),
            in_specs=[
                pl.BlockSpec((rows, depth), lambda i, p: (0, 0)),
                pl.BlockSpec((depth, block), column),
            ],
            out_specs=pl.BlockSpec((1, rows, block), lambda i, p: (i, 0, 0)),
        ),
        compiler_params=pltpu.CompilerParams(vmem_limit_bytes=56 * 2**20),
    )(place, hidden, down)


def pair_sum_body(mine, theirs, out):
    out[...] = (mine[...] + theirs[...].astype(F32)).astype(BF16)


def combine_body(inner, returned, ids, weights, slot, combined_out, squares_out):
    capacity = returned.shape[1]
    rows = ids.shape[0]
    slots = GROUPS * capacity
    chosen = (slot[...] == lax.broadcasted_iota(jnp.int32, (rows, slots), 1)).astype(BF16)
    combined = 0.0
    for twin in range(inner):
        pool = jnp.concatenate([returned[g * inner + twin] for g in range(GROUPS)], axis=0)
        weight = jnp.sum(
            jnp.where(ids[...] % inner == twin, weights[...], 0.0), axis=1, keepdims=True
        )
        combined = combined + contract(chosen, pool, 1, 0) * weight
    combined_out[...] = combined
    squares_out[...] = jnp.sum(combined * combined, axis=1, keepdims=True)


def moe_norm_body(width, combined, squares, gain, out):
    out[...] = (
        combined[...] * lax.rsqrt(squares[...] / width + EPS) * gain[...]
    ).astype(BF16)


def paired_device(
    query_rows,
    key_rows,
    value_rows,
    query_gain,
    key_gain,
    w_out,
    mixer_gain,
    expert_input,
    expert_ids,
    expert_weights,
    input_gain,
    w_gate,
    w_up,
    w_down,
    out_gain,
):
    n_ep, n_tp = lax.axis_size("ep"), lax.axis_size("tp")
    planes = n_ep // 2
    ep, tp = lax.axis_index("ep"), lax.axis_index("tp")
    plane, x = ep // 2, ep % 2
    y, core = tp // 2, tp % 2
    edge = jnp.logical_or(plane == 0, plane == planes - 1)
    place = jnp.stack([ep, x, edge.astype(ep.dtype), y, core, tp]).astype(jnp.int32)

    def swap_x(a):
        return lax.ppermute(a, "ep", [(i, i ^ 1) for i in range(n_ep)])

    def swap_core(a):
        return lax.ppermute(a, "tp", [(i, i ^ 1) for i in range(n_tp)])

    def swap_y(a):
        return lax.ppermute(a, "tp", [(i, i ^ 2) for i in range(n_tp)])

    def swap_z(a, pairs):
        moves = [(2 * s + i, 2 * d + i) for s, d in pairs for i in range(2)]
        return lax.ppermute(a, "ep", moves)

    outer = [(0, 1), (1, 0), (2, 3), (3, 2)]
    middle = [(1, 2), (2, 1)]
    outward = [(1, 0), (2, 3)]

    rows = query_rows.shape[0]
    head_dim = query_gain.shape[0]
    local_kv = key_rows.shape[1] // head_dim
    per = query_rows.shape[1] // key_rows.shape[1]
    groups = local_kv // 2
    tables = turn_tables(rows * n_ep // GRID, head_dim)

    kv_own, kv_other = call(
        prep_kv_body,
        [((2, groups, rows, head_dim), BF16)] * 2,
        [place, key_rows, value_rows, key_gain[None], *tables],
    )
    kv_cross = swap_x(kv_other)
    pair_own = swap_z(kv_own, outer)
    mid_own = swap_z(kv_own, middle)

    width = expert_input.shape[1]
    tokens = expert_input.shape[0]
    capacity = 3 * tokens // 8
    quarter = width // n_tp
    outgoing, slot = call(
        functools.partial(route_body, 2, capacity),
        [((n_ep, capacity, quarter), BF16), ((tokens, 1), jnp.int32)],
        [place, expert_input, expert_ids, input_gain[None]],
    )
    arrived = lax.all_to_all(outgoing, "ep", split_axis=0, concat_axis=0, tiled=True)

    q_own, q_other = call(
        prep_q_body,
        [((groups, per, head_dim, rows), BF16)] * 2,
        [place, query_rows, query_gain[None], *tables],
    )
    q_cross = swap_x(q_other)
    queries = [q_own, q_cross]

    pair_cross = swap_z(kv_cross, outer)
    mid_cross = swap_z(kv_cross, middle)
    far_pair = swap_z(jnp.stack([mid_own, mid_cross]), outward)
    far_mid = swap_z(jnp.stack([pair_own, pair_cross]), middle)
    last_pair = swap_z(far_mid, outward)

    slots = n_ep * capacity
    arrived = arrived.reshape(slots, quarter)
    by_y = swap_y(arrived)
    by_core = swap_core(arrived)
    by_both = swap_core(by_y)

    carry = attend(place, queries, [kv_own, kv_cross], None)
    carry = attend(place, queries, [pair_own, pair_cross], carry)

    hidden = hidden_rows(place, [arrived, by_core, by_y, by_both], w_gate[0], w_up[0], 256)
    down = w_down[0]
    to_core = down_rows(place, hidden, down, True, BF16)
    from_core = swap_core(to_core)
    mine = down_rows(place, hidden, down, False, F32)
    to_y, kept = call(
        cross_sum_body,
        [((slots, quarter), BF16), ((slots, quarter), F32)],
        [place, mine, from_core],
    )
    from_y = swap_y(to_y)

    carry = attend(place, queries, [mid_own, mid_cross, far_pair], carry, pick=True)

    (summed,) = call(pair_sum_body, [((slots, quarter), BF16)], [kept, from_y])
    returned = lax.all_to_all(
        summed.reshape(n_ep, capacity, quarter), "ep", split_axis=0, concat_axis=0, tiled=True
    )

    att_own, att_cross = attend(
        place, queries, [far_mid, last_pair], carry, pick=True, last=True
    )
    half = groups * per * head_dim
    att_back = swap_x(att_cross)
    (base,) = call(
        project_own_body,
        [((rows, w_out.shape[1]), F32)],
        [place, att_own.reshape(half, rows), w_out],
    )
    block = rows // n_tp
    wide = (2, block, w_out.shape[1])
    send, keep = call(
        project_rest_body,
        [(wide, BF16), (wide, F32)],
        [place, att_back.reshape(half, rows), w_out, base],
        scratch_shapes=[pltpu.VMEM(base.shape, F32)],
    )
    got = swap_core(send)
    send_y, keep_y = call(
        cross_sum_body, [(wide[1:], BF16), (wide[1:], F32)], [place, keep, got]
    )
    got_y = swap_y(send_y)

    combined, squares = call(
        functools.partial(combine_body, 2),
        [((tokens, quarter), F32), ((tokens, 1), F32)],
        [returned, expert_ids, expert_weights, slot],
    )
    squares = lax.psum(squares[:, 0], "tp")[:, None]
    (moe_result,) = call(
        functools.partial(moe_norm_body, width),
        [((tokens, quarter), BF16)],
        [combined, squares, out_gain[None]],
    )
    (mixer_result,) = call(
        mixer_norm_body, [(wide[1:], BF16)], [keep_y, got_y, mixer_gain[None]]
    )
    return (mixer_result, moe_result)


def per_device(*arrays):
    query_rows, key_rows, query_gain = arrays[0], arrays[1], arrays[3]
    expert_ids, w_gate = arrays[8], arrays[11]
    n_ep, n_tp = lax.axis_size("ep"), lax.axis_size("tp")
    local_kv = key_rows.shape[1] // query_gain.shape[0]
    experts = w_gate.shape[0] * n_ep
    paired = (
        w_gate.shape[0] == 1
        and experts == 2 * GROUPS
        and expert_ids.shape[1] == 2
        and GROUPS == 4
        and n_tp == 4
        and local_kv % 2 == 0
        and query_rows.shape[0] % GRID == 0
    )
    if paired:
        return paired_device(*arrays)
    return (mixer_half(*arrays[:7]), expert_half(*arrays[7:]))


def solution(mesh):
    return jax.shard_map(
        per_device,
        mesh=mesh,
        in_specs=(
            P("ep", "tp"),
            P("ep", "tp"),
            P("ep", "tp"),
            P(),
            P(),
            P("tp", None),
            P(),
            P("ep", None),
            P("ep", None),
            P("ep", None),
            P(),
            P("ep", None, "tp"),
            P("ep", None, "tp"),
            P("ep", "tp", None),
            P("tp"),
        ),
        out_specs=(P(("ep", "tp"), None), P("ep", "tp")),
        check_vma=False,
    )
```

```python
import functools
import math

import jax
import jax.numpy as jnp
import numpy as np
from jax import lax
from jax.experimental import pallas as pl
from jax.experimental.pallas import tpu as pltpu
from jax.sharding import PartitionSpec as P

GRID = 64
GROUPS = 4


EPS = 1e-06
THETA = 10000.0


def turn_half(half_part, position):
    half_width = half_part.shape[-1]
    frequency = THETA ** (-jnp.arange(0, half_width, 2, dtype=jnp.float32) / half_width)
    angles = position[:, None, None] * frequency[None, None, :]
    cosine = jnp.cos(angles)
    sine_part = jnp.sin(angles)
    first_half = half_part[..., : half_width // 2]
    second = half_part[..., half_width // 2 :]
    return jnp.concatenate(
        [first_half * cosine - second * sine_part, second * cosine + first_half * sine_part],
        axis=-1,
    )


def norm_turn(raw_rows, gain_vec, row_offset):
    row_count = raw_rows.shape[0]
    head_dim = gain_vec.shape[0]
    head_count = raw_rows.shape[1] // head_dim
    by_head = raw_rows.astype(jnp.float32).reshape(row_count, head_count, head_dim)
    scaled = (
        by_head * lax.rsqrt(jnp.mean(by_head * by_head, axis=-1, keepdims=True) + EPS) * gain_vec
    )
    position = row_offset + jnp.arange(row_count, dtype=jnp.int32)
    grid_row = (position // GRID).astype(jnp.float32)
    grid_col = (position % GRID).astype(jnp.float32)
    half_dim = head_dim // 2
    turned = jnp.concatenate(
        [turn_half(scaled[..., :half_dim], grid_row), turn_half(scaled[..., half_dim:], grid_col)],
        axis=-1,
    )
    return turned.reshape(row_count, head_count * head_dim).astype(jnp.bfloat16)


def mixer_half(query_rows, key_rows, value_rows, query_gain, key_gain, w_out, mixer_gain):
    row_count = query_rows.shape[0]
    head_dim = query_gain.shape[0]
    row_offset = lax.axis_index("ep") * row_count
    query_turned = norm_turn(query_rows, query_gain, row_offset)
    key_turned = norm_turn(key_rows, key_gain, row_offset)
    local_kv = key_rows.shape[1] // head_dim
    group_size = query_rows.shape[1] // key_rows.shape[1]
    lane_count = group_size * row_count
    grouped = (
        query_turned.reshape(row_count, local_kv, group_size, head_dim)
        .transpose(1, 2, 0, 3)
        .reshape(local_kv, lane_count, head_dim)
    )
    scaling = head_dim ** (-0.5)

    def attend_block(carry, block_pair):
        running_max, running_sum, weighted = carry
        key_block, value_block = block_pair
        scores = (
            jnp.einsum("gqd,ngd->gqn", grouped, key_block, preferred_element_type=jnp.float32)
            * scaling
        )
        new_max = jnp.maximum(running_max, jnp.max(scores, axis=-1))
        exponent = jnp.exp(scores - new_max[..., None])
        factor = jnp.exp(running_max - new_max)
        running_sum = running_sum * factor + jnp.sum(exponent, axis=-1)
        weighted = weighted * factor[..., None] + jnp.einsum(
            "gqn,ngd->gqd",
            exponent.astype(jnp.bfloat16),
            value_block,
            preferred_element_type=jnp.float32,
        )
        return ((new_max, running_sum, weighted), None)

    initial = (
        jnp.full((local_kv, lane_count), -1e30, jnp.float32),
        jnp.zeros((local_kv, lane_count), jnp.float32),
        jnp.zeros((local_kv, lane_count, head_dim), jnp.float32),
    )
    carry = initial
    key_piece = lax.all_gather(key_turned, "ep", axis=0, tiled=True)
    value_piece = lax.all_gather(value_rows, "ep", axis=0, tiled=True)
    piece_rows = key_piece.shape[0]
    block_rows = 512
    block_count = piece_rows // block_rows
    key_split = key_piece.reshape(block_count, block_rows, local_kv, head_dim)
    value_split = value_piece.reshape(block_count, block_rows, local_kv, head_dim)
    carry, _ = lax.scan(attend_block, carry, (key_split, value_split))
    _, running_sum, weighted = carry
    attended = (weighted / running_sum[..., None]).astype(jnp.bfloat16)
    attended = (
        attended.reshape(local_kv, group_size, row_count, head_dim)
        .transpose(2, 0, 1, 3)
        .reshape(row_count, local_kv * group_size * head_dim)
    )
    mixed_sum = lax.psum_scatter(
        jnp.dot(attended, w_out, preferred_element_type=jnp.float32).astype(jnp.bfloat16),
        "tp",
        scatter_dimension=0,
        tiled=True,
    ).astype(jnp.float32)
    scaled = (
        mixed_sum
        * lax.rsqrt(jnp.mean(mixed_sum * mixed_sum, axis=1, keepdims=True) + EPS)
        * mixer_gain
    )
    return scaled.astype(jnp.bfloat16)


def expert_half(
    expert_input, expert_ids, expert_weights, input_gain, w_gate, w_up, w_down, out_gain
):
    row_count = expert_input.shape[0]
    top_count = expert_ids.shape[1]
    expert_total = w_gate.shape[0] * lax.axis_size("ep")
    inner_count = expert_total // GROUPS
    capacity = 3 * row_count // (4 * inner_count)
    inputs_f = expert_input.astype(jnp.float32)
    normed = (
        inputs_f
        * lax.rsqrt(jnp.mean(inputs_f * inputs_f, axis=1, keepdims=True) + EPS)
        * input_gain
    ).astype(jnp.bfloat16)
    flat_ids = expert_ids.reshape(-1)
    one_hot = (flat_ids[:, None] == jnp.arange(expert_total, dtype=jnp.int32)[None, :]).astype(
        jnp.int32
    )
    earlier = jnp.cumsum(one_hot, axis=0) - one_hot
    rank_in = jnp.sum(earlier * one_hot, axis=1)
    slot_of = flat_ids * capacity + rank_in
    pick_rows = jnp.arange(flat_ids.shape[0], dtype=jnp.int32) // top_count
    source_row = (
        jnp.full((expert_total * capacity,), row_count, jnp.int32).at[slot_of].set(pick_rows)
    )
    padded = jnp.concatenate([normed, jnp.zeros((1, normed.shape[1]), jnp.bfloat16)], axis=0)
    gate_local = w_gate[0]
    up_local = w_up[0]
    down_local = w_down[0]
    outgoing = jnp.take(padded, source_row, axis=0)
    arrived = lax.all_to_all(outgoing, "ep", split_axis=0, concat_axis=0, tiled=True)
    gate_pre = jnp.dot(arrived, gate_local, preferred_element_type=jnp.float32)
    up_pre = jnp.dot(arrived, up_local, preferred_element_type=jnp.float32)
    hidden = (jax.nn.silu(gate_pre) * up_pre).astype(jnp.bfloat16)
    partial_term = jnp.dot(hidden, down_local, preferred_element_type=jnp.float32)
    summed = lax.psum_scatter(
        partial_term.astype(jnp.bfloat16), "tp", scatter_dimension=1, tiled=True
    )
    returned = lax.all_to_all(summed, "ep", split_axis=0, concat_axis=0, tiled=True)
    picked = (
        jnp.take(returned, slot_of, axis=0)
        .reshape(row_count, top_count, returned.shape[1])
        .astype(jnp.float32)
    )
    combined = jnp.sum(picked * expert_weights[:, :, None], axis=1)
    squares = lax.psum(jnp.sum(combined * combined, axis=1), "tp")
    scaled = combined * lax.rsqrt(squares / expert_input.shape[1] + EPS)[:, None] * out_gain
    return scaled.astype(jnp.bfloat16)


VMEM = pl.BlockSpec(memory_space=pltpu.VMEM)
SMEM = pl.BlockSpec(memory_space=pltpu.SMEM)
ANY = pl.BlockSpec(memory_space=pl.ANY)
FLOPS_PER_US = 2e8
F32 = jnp.float32
BF16 = jnp.bfloat16


def contract(lhs, rhs, lhs_dim, rhs_dim):
    return lax.dot_general(
        lhs, rhs, (((lhs_dim,), (rhs_dim,)), ((), ())), preferred_element_type=F32
    )


def cost(us):
    return pl.CostEstimate(flops=int(us * FLOPS_PER_US), bytes_accessed=0, transcendentals=0)


def call(body, outs, args, after=(), us=2.0, specs=None, out_specs=None, **kwargs):
    count = len(args)

    def ordered(*refs):
        body(*refs[:count], *refs[count + len(after) :])

    if specs is None:
        specs = [VMEM] * (count - 1)
    return pl.pallas_call(
        ordered,
        out_shape=[jax.ShapeDtypeStruct(shape, dtype) for shape, dtype in outs],
        in_specs=[SMEM, *specs] + [ANY] * len(after),
        out_specs=out_specs or [VMEM] * len(outs),
        compiler_params=pltpu.CompilerParams(vmem_limit_bytes=56 * 2**20),
        cost_estimate=cost(us),
        **kwargs,
    )(*args, *after)


def blocks(shape, dim):
    block = tuple(1 if i == dim else size for i, size in enumerate(shape))
    return pl.BlockSpec(block, lambda g: tuple(g if i == dim else 0 for i in range(len(shape))))


def as_columns(row):
    return jnp.broadcast_to(row, (128, row.shape[1])).T


def turn_tables(grid_rows, head_dim):
    half = head_dim // 2
    quarter = half // 2
    frequency = np.float32(THETA) ** (
        -np.arange(0, half, 2, dtype=np.float32) / np.float32(half)
    )
    tables = []
    for count, first in ((grid_rows, True), (GRID, False)):
        angles = np.arange(count, dtype=np.float32)[:, None] * frequency[None, :]
        cosine = np.cos(angles.astype(np.float64)).astype(np.float32)
        sine = np.sin(angles.astype(np.float64)).astype(np.float32)
        zero = np.zeros((count, half), np.float32)
        cos_half = np.concatenate([cosine, cosine], axis=1)
        sin_half = np.concatenate([-sine, sine], axis=1)
        pair = [
            np.concatenate([part, zero] if first else [zero, part], axis=1)
            for part in (cos_half, sin_half)
        ]
        tables += pair
    assert tables[0].shape == (grid_rows, 4 * quarter)
    return [jnp.asarray(table) for table in tables]


def turn_one(raw, gain, cosine, sine):
    head_dim = raw.shape[1]
    z = raw.astype(F32)
    z = z * lax.rsqrt(jnp.mean(z * z, axis=1, keepdims=True) + EPS) * gain
    shift = head_dim // 4
    lane = lax.broadcasted_iota(jnp.int32, z.shape, 1)
    partner = jnp.where(
        lane % (2 * shift) < shift,
        pltpu.roll(z, head_dim - shift, 1),
        pltpu.roll(z, shift, 1),
    )
    return z * cosine + partner * sine


def lane_tables(place, row_cos, row_sin, col_cos, col_sin, rows):
    steps = rows // GRID
    base = place[0] * steps
    cosine, sine = [], []
    for step in range(steps):
        cosine.append(row_cos[pl.ds(base + step, 1), :] + col_cos[...])
        sine.append(row_sin[pl.ds(base + step, 1), :] + col_sin[...])
    return jnp.concatenate(cosine, axis=0), jnp.concatenate(sine, axis=0)


def prep_kv_body(place, k, v, gain, rc, rs, cc, cs, own, other):
    rows = k.shape[0]
    head_dim = gain.shape[1]
    groups = own.shape[1]
    cosine, sine = lane_tables(place, rc, rs, cc, cs, rows)
    for out, half in ((own, place[1]), (other, 1 - place[1])):
        for g in range(groups):
            lanes = pl.ds(pl.multiple_of((half * groups + g) * head_dim, head_dim), head_dim)
            out[0, g] = turn_one(k[:, lanes], gain[...], cosine, sine).astype(BF16)
            out[1, g] = v[:, lanes]


def prep_q_body(place, q, gain, rc, rs, cc, cs, own, other):
    rows = q.shape[0]
    head_dim = gain.shape[1]
    groups = own.shape[0]
    per = own.shape[2] // rows
    cosine, sine = lane_tables(place, rc, rs, cc, cs, rows)
    for out, half in ((own, place[1]), (other, 1 - place[1])):
        for g in range(groups):
            for h in range(per):
                head = (half * groups + g) * per + h
                lanes = pl.ds(pl.multiple_of(head * head_dim, head_dim), head_dim)
                turned = turn_one(q[:, lanes], gain[...], cosine, sine)
                out[g, :, h * rows : (h + 1) * rows] = turned.T.astype(BF16)


def attend_body(spec, place, *refs):
    queries, sources, pick, first, last, scale = spec
    q_refs = refs[:queries]
    refs = refs[queries:]
    kv_refs = refs[:sources]
    refs = refs[sources:]
    old = ()
    if not first:
        old, refs = refs[: 3 * queries], refs[3 * queries :]
    end = place[2]

    def pieces(which):
        if not pick:
            return [r[which, 0] for r in kv_refs]
        near, far = kv_refs[:-1], kv_refs[-1]
        chosen = []
        for i in range(2):
            one = near[i][which, 0] if len(near) == 2 else near[0][i, which, 0]
            chosen.append(jnp.where(end > 0, far[i, which, 0], one))
        return chosen

    keys, values = pieces(0), pieces(1)
    for i, q_ref in enumerate(q_refs):
        q = q_ref[0]
        scores = [contract(k, q, 1, 0) for k in keys]
        top = functools.reduce(
            jnp.maximum, [jnp.max(s, axis=0, keepdims=True) for s in scores]
        )
        if not first:
            top = jnp.maximum(top, old[3 * i][0])
        total, weighted = 0.0, 0.0
        for s, v in zip(scores, values):
            p = jnp.exp2(s * scale - top * scale)
            total = total + jnp.sum(p, axis=0, keepdims=True)
            weighted = weighted + contract(v, p.astype(BF16), 0, 0)
        if not first:
            factor = jnp.exp2((old[3 * i][0] - top) * scale)
            total = total + old[3 * i + 1][0] * factor
            weighted = weighted + old[3 * i + 2][0] * factor
        if last:
            attended = (weighted / total).astype(BF16)
            per, rows = refs[i].shape[1], refs[i].shape[3]
            for h in range(per):
                refs[i][0, h] = attended[:, h * rows : (h + 1) * rows]
        else:
            refs[3 * i][0] = top
            refs[3 * i + 1][0] = total
            refs[3 * i + 2][0] = weighted


def attend(place, queries, sources, carry, pick=False, heads=None, after=()):
    groups, head_dim, lanes = queries[0].shape
    scale = head_dim**-0.5 * math.log2(math.e)
    if heads:
        outs = [((groups, heads, head_dim, lanes // heads), BF16)] * len(queries)
    else:
        stat = ((groups, 1, lanes), F32)
        outs = [stat, stat, ((groups, head_dim, lanes), F32)] * len(queries)
    spec = (len(queries), len(sources), pick, carry is None, bool(heads), scale)
    carry = [] if carry is None else list(carry)
    specs = [blocks(a.shape, 0) for a in queries]
    specs += [blocks(a.shape, a.ndim - 3) for a in sources]
    specs += [blocks(a.shape, 0) for a in carry]
    return call(
        functools.partial(attend_body, spec),
        outs,
        [place, *queries, *sources, *carry],
        after,
        us=7.0,
        specs=specs,
        out_specs=[blocks(shape, 0) for shape, _ in outs],
        grid=(groups,),
    )


def project_own_body(place, att, w, out):
    out[...] = contract(att[...], w[...], 0, 0)


def project_rest_body(place, att, w, base, send, near, keep, full):
    full[...] = base[...] + contract(att[...], w[...], 0, 0)
    block = near.shape[0]
    y, core = place[3], place[4]
    for i, there in enumerate((1 - y, y)):
        theirs = pl.ds(pl.multiple_of((2 * there + 1 - core) * block, block), block)
        mine = pl.ds(pl.multiple_of((2 * there + core) * block, block), block)
        send[i] = full[theirs, :].astype(BF16)
        if i == 0:
            near[...] = full[mine, :]
        else:
            keep[...] = full[mine, :]


def project(place, att, w, base, after=()):
    half, rows = att.shape
    width = w.shape[1]
    strip = width // 4
    own = base is None
    lanes = lambda j, p: (0, j)
    if own:
        w_spec = pl.BlockSpec((half, strip), lambda j, p: (p[1], j))
        out_specs, scratch = [pl.BlockSpec((rows, strip), lanes)], []
        shapes = [jax.ShapeDtypeStruct((rows, width), F32)]
    else:
        w_spec = pl.BlockSpec((half, strip), lambda j, p: (1 - p[1], j))
        block = rows // 4
        shapes = [
            jax.ShapeDtypeStruct((2, block, width), BF16),
            jax.ShapeDtypeStruct((block, width), F32),
            jax.ShapeDtypeStruct((block, width), F32),
        ]
        out_specs = [
            pl.BlockSpec((2, block, strip), lambda j, p: (0, 0, j)),
            pl.BlockSpec((block, strip), lanes),
            pl.BlockSpec((block, strip), lanes),
        ]
        scratch = [pltpu.VMEM((rows, strip), F32)]
    args = [att, w] + ([] if own else [base])
    body = project_own_body if own else project_rest_body
    count = 1 + len(args)

    def ordered(*refs):
        body(*refs[:count], *refs[count + len(after) :])

    return pl.pallas_call(
        ordered,
        out_shape=shapes,
        grid_spec=pltpu.PrefetchScalarGridSpec(
            num_scalar_prefetch=1,
            grid=(4,),
            in_specs=[pl.BlockSpec((half, rows), lambda j, p: (0, 0)), w_spec]
            + ([] if own else [pl.BlockSpec((rows, strip), lanes)])
            + [ANY] * len(after),
            out_specs=out_specs,
            scratch_shapes=scratch,
        ),
        compiler_params=pltpu.CompilerParams(vmem_limit_bytes=56 * 2**20),
        cost_estimate=cost(4.0),
    )(place, *args, *after)


def route_body(inner, capacity, place, x, ids, gain, out, slot_out):
    rows, _ = x.shape
    quarter = out.shape[2]
    xf = x[...].astype(F32)
    inverse = lax.rsqrt(jnp.mean(xf * xf, axis=1, keepdims=True) + EPS)
    lanes = pl.ds(pl.multiple_of(place[5] * quarter, quarter), quarter)
    normed = (x[:, lanes].astype(F32) * inverse * gain[:, lanes]).astype(BF16)
    group = as_columns((ids[0:1, :] // inner).astype(F32)).astype(jnp.int32)
    in_group = group == lax.broadcasted_iota(jnp.int32, (rows, 128), 1)
    earlier = lax.broadcasted_iota(jnp.int32, (rows, rows), 0) > lax.broadcasted_iota(
        jnp.int32, (rows, rows), 1
    )
    rank = contract(earlier.astype(BF16), in_group.astype(BF16), 1, 0)
    rank = jnp.sum(jnp.where(in_group, rank, 0.0), axis=1, keepdims=True).astype(jnp.int32)
    slot = group[:, 0:1] * capacity + rank
    slot_out[...] = slot
    slots = GROUPS * capacity
    chosen = (slot == lax.broadcasted_iota(jnp.int32, (rows, slots), 1)).astype(BF16)
    sorted_rows = contract(chosen, normed, 0, 0).astype(BF16)
    for g in range(GROUPS):
        for twin in range(inner):
            out[g * inner + twin] = sorted_rows[g * capacity : (g + 1) * capacity]


def hidden_body(place, own, by_core, by_y, by_both, gate, up, *rest):
    out = rest[-1]
    quarter = own.shape[1]
    y, core = place[3], place[4]
    order = (2 * y + core, 2 * y + 1 - core, 2 * (1 - y) + core, 2 * (1 - y) + 1 - core)
    gate_pre, up_pre = 0.0, 0.0
    for ref, index in zip((own, by_core, by_y, by_both), order):
        part = pl.ds(pl.multiple_of(index * quarter, quarter), quarter)
        rows = ref[...]
        gate_pre = gate_pre + contract(rows, gate[part, :], 1, 0)
        up_pre = up_pre + contract(rows, up[part, :], 1, 0)
    out[...] = (gate_pre / (1.0 + jnp.exp(-gate_pre)) * up_pre).astype(BF16)


def hidden_rows(place, pieces, gate, up, block, after):
    rows, quarter = pieces[0].shape
    depth, width = gate.shape
    whole = pl.BlockSpec((rows, quarter), lambda i, p: (0, 0))
    strip = pl.BlockSpec((depth, block), lambda i, p: (0, i))
    return pl.pallas_call(
        hidden_body,
        out_shape=jax.ShapeDtypeStruct((rows, width), BF16),
        grid_spec=pltpu.PrefetchScalarGridSpec(
            num_scalar_prefetch=1,
            grid=(width // block,),
            in_specs=[whole] * 4 + [strip] * 2 + [ANY] * len(after),
            out_specs=pl.BlockSpec((rows, block), lambda i, p: (0, i)),
        ),
        compiler_params=pltpu.CompilerParams(vmem_limit_bytes=56 * 2**20),
        cost_estimate=cost(9.0),
    )(place, *pieces, gate, up, *after)


def theirs_body(place, hidden, down, out):
    out[0] = contract(hidden[...], down[...], 1, 0).astype(BF16)


def mine_body(place, hidden, down, got, *rest):
    near, keep = rest[-2:]
    full = contract(hidden[...], down[...], 1, 0) + got[0].astype(F32)

    @pl.when(pl.program_id(0) == 0)
    def _():
        near[...] = full.astype(BF16)

    @pl.when(pl.program_id(0) == 1)
    def _():
        keep[...] = full


def down_theirs(place, hidden, down):
    rows, depth = hidden.shape
    block = down.shape[1] // 4
    there = lambda i, p: i * p[3] + (1 - i) * (1 - p[3])
    return pl.pallas_call(
        theirs_body,
        out_shape=jax.ShapeDtypeStruct((2, rows, block), BF16),
        grid_spec=pltpu.PrefetchScalarGridSpec(
            num_scalar_prefetch=1,
            grid=(2,),
            in_specs=[
                pl.BlockSpec((rows, depth), lambda i, p: (0, 0)),
                pl.BlockSpec((depth, block), lambda i, p: (0, 2 * there(i, p) + 1 - p[4])),
            ],
            out_specs=pl.BlockSpec((1, rows, block), lambda i, p: (i, 0, 0)),
        ),
        compiler_params=pltpu.CompilerParams(vmem_limit_bytes=56 * 2**20),
        cost_estimate=cost(5.0),
    )(place, hidden, down)


def down_mine(place, hidden, down, got, after):
    rows, depth = hidden.shape
    block = down.shape[1] // 4
    there = lambda i, p: i * p[3] + (1 - i) * (1 - p[3])
    return pl.pallas_call(
        mine_body,
        out_shape=[
            jax.ShapeDtypeStruct((rows, block), BF16),
            jax.ShapeDtypeStruct((rows, block), F32),
        ],
        grid_spec=pltpu.PrefetchScalarGridSpec(
            num_scalar_prefetch=1,
            grid=(2,),
            in_specs=[
                pl.BlockSpec((rows, depth), lambda i, p: (0, 0)),
                pl.BlockSpec((depth, block), lambda i, p: (0, 2 * there(i, p) + p[4])),
                pl.BlockSpec((1, rows, block), lambda i, p: (i, 0, 0)),
            ]
            + [ANY] * len(after),
            out_specs=[pl.BlockSpec((rows, block), lambda i, p: (0, 0))] * 2,
        ),
        compiler_params=pltpu.CompilerParams(vmem_limit_bytes=56 * 2**20),
        cost_estimate=cost(5.0),
    )(place, hidden, down, got, *after)


def combine_body(inner, place, returned, ids, weights, slot, combined_out, squares_out):
    capacity = returned.shape[1]
    rows = slot.shape[0]
    slots = GROUPS * capacity
    chosen = (slot[...] == lax.broadcasted_iota(jnp.int32, (rows, slots), 1)).astype(BF16)
    combined = 0.0
    for twin in range(inner):
        pool = jnp.concatenate([returned[g * inner + twin] for g in range(GROUPS)], axis=0)
        weight = jnp.sum(
            jnp.where(ids[...] % inner == twin, weights[...], 0.0), axis=0, keepdims=True
        )
        combined = combined + contract(chosen, pool, 1, 0) * as_columns(weight)[:, 0:1]
    combined_out[...] = combined
    squares = jnp.sum(combined * combined, axis=1, keepdims=True)
    squares_out[...] = jnp.broadcast_to(squares, (rows, 128)).T[:8]


def finish_body(
    width, place, combined, one, two, three, four, out_gain, keep, got, got_y, mixer_gain, moe, mixer
):
    squares = (one[...] + two[...] + three[...] + four[...])[0:1]
    inverse = lax.rsqrt(squares / width + EPS)
    moe[...] = (combined[...] * as_columns(inverse)[:, 0:1] * out_gain[...]).astype(BF16)
    mixed = keep[...] + got[1].astype(F32) + got_y[...].astype(F32)
    mean = jnp.mean(mixed * mixed, axis=1, keepdims=True)
    mixer[...] = (mixed * lax.rsqrt(mean + EPS) * mixer_gain[...]).astype(BF16)


def paired_device(
    query_rows,
    key_rows,
    value_rows,
    query_gain,
    key_gain,
    w_out,
    mixer_gain,
    expert_input,
    expert_ids,
    expert_weights,
    input_gain,
    w_gate,
    w_up,
    w_down,
    out_gain,
):
    n_ep, n_tp = lax.axis_size("ep"), lax.axis_size("tp")
    planes = n_ep // 2
    ep, tp = lax.axis_index("ep"), lax.axis_index("tp")
    plane, x = ep // 2, ep % 2
    y, core = tp // 2, tp % 2
    edge = jnp.logical_or(plane == 0, plane == planes - 1)
    place = jnp.stack([ep, x, edge.astype(ep.dtype), y, core, tp]).astype(jnp.int32)

    def swap_ep(a, pairs):
        return lax.ppermute(a, "ep", pairs)

    def swap_tp(a, bits):
        return lax.ppermute(a, "tp", [(i, i ^ bits) for i in range(n_tp)])

    def swap_x(a):
        return swap_ep(a, [(i, i ^ 1) for i in range(n_ep)])

    def swap_z(a, pairs):
        return swap_ep(a, [(2 * s + i, 2 * d + i) for s, d in pairs for i in range(2)])

    def exchange(a):
        return lax.all_to_all(a, "ep", split_axis=0, concat_axis=0, tiled=True)

    outer = [(0, 1), (1, 0), (2, 3), (3, 2)]
    middle = [(1, 2), (2, 1)]
    outward = [(1, 0), (2, 3)]

    rows = query_rows.shape[0]
    head_dim = query_gain.shape[0]
    local_kv = key_rows.shape[1] // head_dim
    per = query_rows.shape[1] // key_rows.shape[1]
    groups = local_kv // 2
    tables = turn_tables(rows * n_ep // GRID, head_dim)

    kv_own, kv_other = call(
        prep_kv_body,
        [((2, groups, rows, head_dim), BF16)] * 2,
        [place, key_rows, value_rows, key_gain[None], *tables],
    )
    kv_cross = swap_x(kv_other)
    pair_own = swap_z(kv_own, outer)
    mid_own = swap_z(kv_own, middle)

    width = expert_input.shape[1]
    tokens = expert_input.shape[0]
    capacity = 3 * tokens // 8
    quarter = width // n_tp
    ids, weights = expert_ids.T, expert_weights.T
    outgoing, slot = call(
        functools.partial(route_body, 2, capacity),
        [((n_ep, capacity, quarter), BF16), ((tokens, 1), jnp.int32)],
        [place, expert_input, ids, input_gain[None]],
        after=[kv_own],
    )
    arrived = exchange(outgoing)

    q_own, q_other = call(
        prep_q_body,
        [((groups, head_dim, per * rows), BF16)] * 2,
        [place, query_rows, query_gain[None], *tables],
        after=[outgoing],
        us=4.0,
    )
    q_cross = swap_x(q_other)
    queries = [q_own, q_cross]

    pair_cross = swap_z(kv_cross, outer)
    mid_cross = swap_z(kv_cross, middle)
    far_pair = swap_z(jnp.stack([mid_own, mid_cross]), outward)
    far_mid = swap_z(jnp.stack([pair_own, pair_cross]), middle)
    last_pair = swap_z(far_mid, outward)

    slots = n_ep * capacity
    arrived = arrived.reshape(slots, quarter)
    by_y = swap_tp(arrived, 2)
    by_core = swap_tp(arrived, 1)
    by_both = swap_tp(by_y, 1)

    carry = attend(place, queries, [kv_own, kv_cross], None)
    carry = attend(place, queries, [pair_own, pair_cross], carry)
    hidden = hidden_rows(
        place, [arrived, by_core, by_y, by_both], w_gate[0], w_up[0], 256, [carry[0]]
    )
    to_core = down_theirs(place, hidden, w_down[0])
    from_core = swap_tp(to_core, 1)
    carry = attend(place, queries, [mid_own, mid_cross, far_pair], carry, True, None, [to_core])
    to_y, kept = down_mine(place, hidden, w_down[0], from_core, [carry[0]])
    from_y = swap_tp(to_y, 2)
    att_own, att_cross = attend(place, queries, [far_mid, last_pair], carry, True, per, [to_y])
    half = groups * per * head_dim
    att_back = swap_x(att_cross)
    (base,) = project(place, att_own.reshape(half, rows), w_out, None)
    kept, _ = lax.optimization_barrier((kept, base))
    summed = (kept + from_y.astype(F32)).astype(BF16)
    returned = exchange(summed.reshape(n_ep, capacity, quarter))

    send, near, keep = project(place, att_back.reshape(half, rows), w_out, base)
    got = swap_tp(send, 1)
    to_near = (near + got[0].astype(F32)).astype(BF16)
    got_y = swap_tp(to_near, 2)
    combined, squares = call(
        functools.partial(combine_body, 2),
        [((tokens, quarter), F32), ((8, tokens), F32)],
        [place, returned, ids, weights, slot],
        after=[send],
    )
    others = [swap_tp(squares, bits) for bits in (1, 2, 3)]
    moe_result, mixer_result = call(
        functools.partial(finish_body, width),
        [((tokens, quarter), BF16), ((rows // n_tp, w_out.shape[1]), BF16)],
        [place, combined, squares, *others, out_gain[None], keep, got, got_y, mixer_gain[None]],
    )
    return (mixer_result, moe_result)


def per_device(*arrays):
    query_rows, key_rows, query_gain = arrays[0], arrays[1], arrays[3]
    expert_ids, w_gate = arrays[8], arrays[11]
    n_ep, n_tp = lax.axis_size("ep"), lax.axis_size("tp")
    local_kv = key_rows.shape[1] // query_gain.shape[0]
    experts = w_gate.shape[0] * n_ep
    paired = (
        w_gate.shape[0] == 1
        and experts == 2 * GROUPS
        and expert_ids.shape[1] == 2
        and GROUPS == 4
        and n_tp == 4
        and local_kv % 2 == 0
        and query_rows.shape[0] % GRID == 0
    )
    if paired:
        return paired_device(*arrays)
    return (mixer_half(*arrays[:7]), expert_half(*arrays[7:]))


def solution(mesh):
    return jax.shard_map(
        per_device,
        mesh=mesh,
        in_specs=(
            P("ep", "tp"),
            P("ep", "tp"),
            P("ep", "tp"),
            P(),
            P(),
            P("tp", None),
            P(),
            P("ep", None),
            P("ep", None),
            P("ep", None),
            P(),
            P("ep", None, "tp"),
            P("ep", None, "tp"),
            P("ep", "tp", None),
            P("tp"),
        ),
        out_specs=(P(("ep", "tp"), None), P("ep", "tp")),
        check_vma=False,
    )
```
